32 devices in a mesh: sp: 8 (over z, core), tp: 4 (over y, x).
Axes of the slice: x: 2, y: 2, z: 4, core: 2. Of those that a mesh axis runs over, the one named last changes fastest.
Arguments:
- residual: bfloat16 [2048, 4096], P('sp', 'tp'), may hold values from -6 to 6
- pool_in: bfloat16 [2048, 2048], P('sp', 'tp'), may hold values from -6 to 6
- docs: int32 [2048], P('sp'), may hold values from 0 to 3, never falling along the last dimension, each value on 1 to 1024 neighbouring positions
- pool_weight: bfloat16 [16, 128, 128], P('tp'), may hold values from -0.5 to 0.5
- pool_gain: float32 [2048], P('tp'), may hold values from 0.1 to 1.9
- out_weight: bfloat16 [2048, 4096], P(None, 'tp'), may hold values from -0.125 to 0.125
- norm_gain: float32 [4096], replicated, may hold values from 0.1 to 1.9
- routes: int32 [2048, 2], P('sp'), may hold values from 0 to 7, all different within a row; in each aligned block of 256 rows (0 to 255, 256 to 511, ...) at most 96 rows name the same one
- route_weights: float32 [2048, 2], P('sp'), may hold values from 0.25 to 1
- w_gate: bfloat16 [8, 4096, 2048], P('sp', None, 'tp'), may hold values from -0.09375 to 0.09375
- w_up: bfloat16 [8, 4096, 2048], P('sp', None, 'tp'), may hold values from -0.09375 to 0.09375
- w_down: bfloat16 [8, 2048, 4096], P('sp', None, 'tp'), may hold values from -0.125 to 0.125
Outputs:
- layer_out: bfloat16 [2048, 4096], P('sp', 'tp')
The draws below stay inside these ranges and needn't reach their ends.
Inputs may be any that keep to these rules, and one draw needn't show every extreme that they name: `docs`: document numbers never fall along the sequence; each document has at most 1024 positions. `routes`: each token names 2 different experts; among the tokens of one index of sp (aligned blocks of 256 rows) no expert is named more than 96 times, a bound that some block reaches.
All inputs are finite; a program needn't handle non-finite values.
Results may differ from the reference program's by a relative error of at most 0.012.
Values may be sent and summed in bfloat16 or wider, within the bound.
A program may use at most 64 MiB of HBM per device.

```python
import math
import jax
import jax.numpy as jnp
import numpy as np
from jax import lax

D = 4096
DFF = 2048
GD = 128
POOL_GROUPS = 16
TOPK = 2
TOK_DEV = 256
POOL_WIDTH = 2048
EXPERTS = 8
TOKENS = 2048
CAP = 96
DOCS = 4
DOC_MOST = 1024
N_SP = 8


def steps_of(stream_key, dims, split, least, top_value):
    factor_of, own = 1.0, jax.random.fold_in(stream_key, 6)
    for axis_at, parts in split:
        heights = jnp.exp(jax.random.uniform(jax.random.fold_in(own, axis_at), (parts,), jnp.float32, least / len(split), top_value / len(split)))
        factor_of = factor_of * jnp.repeat(heights, dims[axis_at] // parts).reshape([-1 if axis == axis_at else 1 for axis in range(len(dims))])
    return factor_of


def length_profile(number_of, total, most, slope):
    loads = [(1 << 20) // math.isqrt(rank ** slope) + 1 for rank in range(2, number_of + 1)]
    spare, given = total - most - (number_of - 1), [1] * (number_of - 1)
    while spare > 0:
        movable = [i for i in range(number_of - 1) if given[i] < most]
        whole, remaining = sum([loads[i] for i in movable]), spare
        for i in movable:
            extra = min(most - given[i], max(1, remaining * loads[i] // whole), spare)
            given[i] = given[i] + extra
            spare = spare - extra
    return np.array([most] + given)


def uneven_parts(key, count, total, bound, lean):
    if count == 2:
        one = jax.random.randint(key, (), max(1, total - bound), min(bound, total - 1) + 1)
        return jnp.stack([one, total - one])
    sizes = jnp.asarray(length_profile(count, total, bound, lean), jnp.int32)
    twos = (count - 1) // 2
    giver, sink = sizes[1:1 + 2 * twos:2], sizes[2:2 + 2 * twos:2]
    room = jnp.minimum(giver - 1, bound - sink)
    moved = jax.random.randint(jax.random.fold_in(key, 1), (twos,), 0, 1 << 20) % (room + 1)
    sizes = sizes.at[1:1 + 2 * twos:2].set(giver - moved).at[2:2 + 2 * twos:2].set(sink + moved)
    return sizes[jax.random.permutation(jax.random.fold_in(key, 2), count)]


def routed_block(rng, own, number, rows, amount, top, limit, slope):
    ranking = jax.random.permutation(rng, amount)
    crowded, common = load_shares(amount, rows * top, limit, slope, True), load_shares(amount, rows * top, limit, slope, False)
    places = jnp.arange(amount)

    def named(tallies, turn):
        used = int((tallies > 0).sum())
        fixed = max(1, used // 4)
        moved = fixed + (places - fixed + turn * (used - fixed)) % max(1, amount - fixed)
        return jnp.zeros((amount,), jnp.int32).at[ranking[jnp.where(places < fixed, places, moved)]].set(jnp.asarray(tallies, jnp.int32))

    tallies = jnp.where(number % 4 == 0, named(crowded, number // 4), named(common, number - number // 4 - 1))
    mixed = jax.random.permutation(jax.random.fold_in(own, 3), amount)
    giver, sink = mixed[0:amount // 2 * 2:2], mixed[1:amount // 2 * 2:2]
    slack = jnp.minimum(tallies[giver] - 1, limit - tallies[sink]) // 2
    slack = jnp.where((giver == ranking[0]) | (sink == ranking[0]) | (tallies[sink] == 0), 0, jnp.maximum(slack, 0))
    moved = jax.random.randint(jax.random.fold_in(own, 4), (amount // 2,), 0, 1 << 20) % (slack + 1)
    tallies = tallies.at[giver].add(-moved).at[sink].add(moved)
    items = jnp.searchsorted(jnp.cumsum(tallies), jnp.arange(rows * top), side="right").astype(jnp.int32)
    grid = items.reshape(top, rows).T
    grid = grid[jax.random.permutation(jax.random.fold_in(own, 1), rows)]
    turn = jax.random.randint(jax.random.fold_in(own, 2), (rows, 1), 0, top)
    return jnp.take_along_axis(grid, (jnp.arange(top)[None, :] + turn) % top, axis=1)


def load_shares(number_of, total, reach, slope, full):
    portions = [(1 << 20) // math.isqrt(standing ** slope) + 1 for standing in range(1, number_of + 1)]
    largest = reach if full else min(reach, max(-(-total // number_of), total * portions[0] // sum(portions)))
    least = 1 if total - largest >= number_of - 1 else 0
    holding, spare = [largest] + [least] * (number_of - 1), total - largest - least * (number_of - 1)
    while spare > 0:
        candidates = [i for i in range(1, number_of) if holding[i] < largest] or [i for i in range(1, number_of) if holding[i] < reach]
        whole, budget = sum([portions[i] for i in candidates]), spare
        for i in candidates:
            addition = min(reach - holding[i], max(1, budget * portions[i] // whole), spare)
            holding[i] = holding[i] + addition
            spare = spare - addition
    return np.array(holding)


def bell_draw(own_key, extent, deviation, most, shards=(), held_as=jnp.bfloat16):
    drawn = deviation * jax.random.normal(own_key, extent, jnp.float32)
    if shards:
        drawn = drawn * steps_of(own_key, extent, shards, -0.22, 0.18)
    return jnp.clip(drawn, -most, most).astype(held_as)


def setup_inputs(seed: int = 0) -> dict:
    key_list = jax.random.split(jax.random.key(seed), 13)
    residual = bell_draw(key_list[0], (TOKENS, D), 1.0, 6.0, ((0, 8), (1, 4)))
    pool_in = bell_draw(key_list[1], (TOKENS, POOL_WIDTH), 1.0, 6.0, ((0, 8), (1, 4)))
    docs = jnp.searchsorted(jnp.cumsum(uneven_parts(key_list[2], DOCS, TOKENS, DOC_MOST, 1)), jnp.arange(TOKENS), side="right").astype(jnp.int32)
    pool_weight = bell_draw(key_list[3], (POOL_GROUPS, GD, GD), GD ** -0.5, 0.5, ((0, 4),))
    pool_gain = jnp.clip(1.0 + 0.18 * jax.random.normal(key_list[4], (POOL_WIDTH,), jnp.float32), 0.1, 1.9)
    out_weight = bell_draw(key_list[5], (POOL_WIDTH, D), POOL_WIDTH ** -0.5, 0.125, ((1, 4),))
    norm_gain = jnp.clip(1.0 + 0.18 * jax.random.normal(key_list[6], (D,), jnp.float32), 0.1, 1.9)
    routes_keys = jax.random.split(jax.random.fold_in(key_list[7], 1), TOKENS // TOK_DEV)
    routes_turns = jax.random.permutation(jax.random.fold_in(key_list[7], 3), TOKENS // TOK_DEV)
    routes = jax.vmap(lambda own, number: routed_block(jax.random.fold_in(key_list[7], 2), own, number, TOK_DEV, EXPERTS, TOPK, CAP, 1))(routes_keys, routes_turns).reshape((TOKENS, TOPK))
    route_weights = jnp.clip(0.25 + 0.75 * jax.random.uniform(key_list[8], (TOKENS, TOPK), jnp.float32) ** steps_of(key_list[8], (TOKENS, TOPK), ((0, 8),), -0.2, 0.2), 0.25, 1.0)
    w_gate = bell_draw(key_list[9], (EXPERTS, D, DFF), D ** -0.5, 0.09375, ((0, 8), (2, 4)))
    w_up = bell_draw(key_list[10], (EXPERTS, D, DFF), D ** -0.5, 0.09375, ((0, 8), (2, 4)))
    w_down = bell_draw(key_list[11], (EXPERTS, DFF, D), DFF ** -0.5, 0.125, ((0, 8), (2, 4)))
    return {"residual": residual, "pool_in": pool_in, "docs": docs, "pool_weight": pool_weight, "pool_gain": pool_gain, "out_weight": out_weight, "norm_gain": norm_gain, "routes": routes, "route_weights": route_weights, "w_gate": w_gate, "w_up": w_up, "w_down": w_down}


EPS = 1e-06

def pool_mix(pool_in, docs, pool_weight, pool_gain):
    length = pool_in.shape[0]
    values = pool_in.astype(jnp.float32)
    places = jnp.arange(length)
    group_of = jnp.arange(POOL_WIDTH) // GD
    span = 2 ** (1 + group_of % 4)
    totals = jnp.zeros((length, POOL_WIDTH), jnp.float32)
    counts = jnp.zeros((length, POOL_WIDTH), jnp.float32)
    for offset in range(16):
        shifted = jnp.pad(values, ((offset, 0), (0, 0)))[:length]
        prior = jnp.pad(docs, (offset, 0))[:length]
        same = ((places >= offset) & (prior == docs)).astype(jnp.float32)[:, None]
        inside = (offset < span).astype(jnp.float32)[None, :]
        weight = same * inside
        totals = totals + weight * shifted
        counts = counts + weight
    diff = (totals / counts - values).astype(jnp.bfloat16)
    mixed = jnp.einsum('tgc,gcd->tgd', diff.reshape(length, POOL_GROUPS, GD).astype(jnp.float32), pool_weight.astype(jnp.float32))
    return (mixed.reshape(length, POOL_WIDTH) * pool_gain).astype(jnp.bfloat16)

def expert_apply(packed):
    rows, gate_w, up_w, down_w = packed
    gate = jnp.dot(rows, gate_w, preferred_element_type=jnp.float32)
    up = jnp.dot(rows, up_w, preferred_element_type=jnp.float32)
    act = (jax.nn.silu(gate) * up).astype(jnp.bfloat16)
    return jnp.dot(act, down_w, preferred_element_type=jnp.float32).astype(jnp.bfloat16)

def reference(residual, pool_in, docs, pool_weight, pool_gain, out_weight, norm_gain, routes, route_weights, w_gate, w_up, w_down):
    pooled = pool_mix(pool_in, docs, pool_weight, pool_gain)
    proj = jnp.dot(pooled, out_weight, preferred_element_type=jnp.float32)
    updated = (residual.astype(jnp.float32) + proj).astype(jnp.bfloat16)
    upf = updated.astype(jnp.float32)
    normed = (upf * lax.rsqrt(lax.optimization_barrier(jnp.mean(upf * upf, axis=1, keepdims=True)) + EPS) * norm_gain).astype(jnp.bfloat16)
    ids = routes.reshape(N_SP, TOK_DEV * TOPK)
    onehot = (ids[:, :, None] == jnp.arange(EXPERTS)[None, None, :]).astype(jnp.int32)
    rank = lax.optimization_barrier(jnp.sum(onehot * (jnp.cumsum(onehot, axis=1) - 1), axis=2))
    blocks = jnp.arange(N_SP)[:, None]
    flat = (ids * (N_SP * CAP) + blocks * CAP + rank).reshape(-1).astype(jnp.int32)
    source = (blocks * TOK_DEV + jnp.arange(TOK_DEV * TOPK)[None, :] // TOPK).reshape(-1).astype(jnp.int32)
    buffer = jnp.zeros((EXPERTS * N_SP * CAP, D), jnp.bfloat16).at[flat].set(normed[source])
    results = lax.map(expert_apply, (buffer.reshape(EXPERTS, N_SP * CAP, D), w_gate, w_up, w_down))
    picked = results.reshape(EXPERTS * N_SP * CAP, D)[flat].reshape(TOKENS, TOPK, D)
    combined = upf + lax.optimization_barrier(jnp.sum(route_weights[:, :, None] * picked.astype(jnp.float32), axis=1))
    return combined.astype(jnp.bfloat16)
```

```python
import functools

import jax
import jax.numpy as jnp
from jax import lax
from jax.experimental import pallas as pl
from jax.experimental.pallas import tpu as pltpu
from jax.sharding import PartitionSpec as P

GD = 128
TOPK = 2
EXP_DEV = 1


EPS = 1e-06


def shifted_2(shard, axis, by):
    size = lax.axis_size(axis)
    pairs = [(i, i + by) for i in range(size) if 0 <= i + by < size]
    return lax.ppermute(shard, axis, pairs)


MESH = pl.DeviceIdType.MESH
CORES = 2


def remote(src, dst, send_sem, recv_sem, device):
    return pltpu.make_async_remote_copy(
        src_ref=src,
        dst_ref=dst,
        send_sem=send_sem,
        recv_sem=recv_sem,
        device_id=device,
        device_id_type=MESH,
    )


def greet(devices):
    barrier = pltpu.get_barrier_semaphore()
    for device in devices:
        pl.semaphore_signal(barrier, inc=1, device_id=device, device_id_type=MESH)
    pl.semaphore_wait(barrier, len(devices))


def project_kernel(
    n_tp,
    pooled,
    residual,
    gain,
    weight_hbm,
    updated,
    normed,
    gathered,
    weight,
    mine,
    sums,
    weight_sem,
    send_sem,
    recv_sem,
    sums_send,
    sums_recv,
):
    sp, tp = lax.axis_index("sp"), lax.axis_index("tp")
    width = pooled.shape[1]
    cols = residual.shape[1]
    load = pltpu.make_async_copy(weight_hbm, weight, weight_sem)
    load.start()
    peers = [lax.rem(tp + j, n_tp) for j in range(1, n_tp)]
    greet([(sp, peer) for peer in peers])
    sends = []
    for j, peer in enumerate(peers):
        sends.append(
            remote(pooled, gathered.at[tp], send_sem.at[j], recv_sem.at[tp], (sp, peer))
        )
        sends[-1].start()
    load.wait()

    def part(block, owner):
        rows = weight[pl.ds(pl.multiple_of(owner * width, width), width), :]
        return jnp.dot(block, rows, preferred_element_type=jnp.float32)

    total = part(pooled[...], tp)
    for j in range(1, n_tp):
        owner = lax.rem(tp + n_tp - j, n_tp)
        remote(
            pooled, gathered.at[owner], send_sem.at[0], recv_sem.at[owner], (sp, owner)
        ).wait_recv()
        total = total + part(gathered[owner], owner)
    new = (residual[...].astype(jnp.float32) + total).astype(jnp.bfloat16)
    updated[...] = new
    upf = new.astype(jnp.float32)
    squares = jnp.sum(upf * upf, axis=1, keepdims=True)
    own = jnp.broadcast_to(squares, (squares.shape[0], 128)).T[0:8]
    mine[...] = own
    small = []
    for j, peer in enumerate(peers):
        small.append(
            remote(mine, sums.at[tp], sums_send.at[j], sums_recv.at[tp], (sp, peer))
        )
        small[-1].start()
    for j in range(1, n_tp):
        owner = lax.rem(tp + n_tp - j, n_tp)
        remote(
            mine, sums.at[owner], sums_send.at[0], sums_recv.at[owner], (sp, owner)
        ).wait_recv()
        own = own + sums[owner]
    scale = lax.rsqrt(own / (cols * n_tp) + EPS)
    column = jnp.broadcast_to(scale[0:1], (128, scale.shape[1])).T[:, 0:1]
    normed[...] = (upf * column * gain[...]).astype(jnp.bfloat16)
    for copy in sends + small:
        copy.wait_send()


def experts_kernel(
    n_sp,
    n_tp,
    send,
    gate_hbm,
    up_hbm,
    down_hbm,
    out,
    rows,
    act,
    prod,
    w_gate,
    w_up,
    w_down,
    load_sem,
    d_send,
    d_recv,
    f_send,
    f_recv,
    a_send,
    a_recv,
    r_send,
    r_recv,
):
    sp, tp = lax.axis_index("sp"), lax.axis_index("tp")
    chips = n_sp // CORES
    my_chip, my_core = sp // CORES, sp % CORES
    cap, cols = send.shape[2], send.shape[3]
    hidden = act.shape[4]
    relay = n_tp == 4
    flat = CORES * cap

    loads = [
        pltpu.make_async_copy(gate_hbm, w_gate, load_sem.at[0]),
        pltpu.make_async_copy(up_hbm, w_up, load_sem.at[1]),
        pltpu.make_async_copy(down_hbm, w_down, load_sem.at[2]),
    ]
    for copy in loads:
        copy.start()
    greet(
        [(lax.rem(sp + j, n_sp), tp) for j in range(1, n_sp)]
        + [(sp, lax.rem(tp + j, n_tp)) for j in range(1, n_tp)]
    )

    def turn(k):
        odd = k % 2
        return (odd * ((k + 1) // 2) + (1 - odd) * (chips - k // 2)) % chips

    def dispatch(chip, core):
        return remote(
            send.at[chip, core],
            rows.at[my_chip, tp, my_core],
            d_send.at[chip * CORES + core],
            d_recv.at[sp],
            (chip * CORES + core, tp),
        )

    own = pltpu.make_async_copy(
        send.at[my_chip, my_core], rows.at[my_chip, tp, my_core], d_recv.at[sp]
    )
    own.start()
    dispatch(my_chip, 1 - my_core).start()

    @pl.loop(1, chips)
    def _(k):
        chip = (my_chip + turn(k)) % chips
        for core in range(CORES):
            dispatch(chip, core).start()

    def spread(buf, chip, ssem, rsem):
        if relay:
            near = (2 * (tp // 2) + 1 - tp % 2, (tp + 2) % 4)
        else:
            near = [(tp + j) % n_tp for j in range(1, n_tp)]
        return [
            remote(buf.at[chip, tp], buf.at[chip, tp], ssem.at[chip, j], rsem.at[chip, tp], (sp, peer))
            for j, peer in enumerate(near)
        ]

    across = 2 * (tp // 2) + 1 - tp % 2
    along = (tp + 2) % 4

    def relays(buf, chip, ssem, rsem):
        return [
            remote(
                buf.at[chip, across, 0],
                buf.at[chip, across, 0],
                ssem.at[chip, 2],
                rsem.at[chip, n_tp],
                (sp, along),
            ),
            remote(
                buf.at[chip, along, 1],
                buf.at[chip, along, 1],
                ssem.at[chip, 3],
                rsem.at[chip, n_tp + 1],
                (sp, across),
            ),
        ]

    def arrive(buf, chip, peer, ssem, rsem):
        remote(
            buf.at[chip, peer], buf.at[chip, peer], ssem.at[chip, 0], rsem.at[chip, peer], (sp, peer)
        ).wait_recv()

    def pass_on(buf, chip, ssem, rsem):
        if relay:
            first, second = relays(buf, chip, ssem, rsem)
            arrive(buf, chip, across, ssem, rsem)
            first.start()
            arrive(buf, chip, along, ssem, rsem)
            second.start()

    def complete(buf, chip, ssem, rsem):
        if relay:
            far = 3 - tp
            for half, peer in ((0, along), (1, across)):
                remote(
                    buf.at[chip, far, half],
                    buf.at[chip, far, half],
                    ssem.at[chip, 0],
                    rsem.at[chip, n_tp + half],
                    (sp, peer),
                ).wait_recv()
        else:
            for j in range(1, n_tp):
                arrive(buf, chip, (tp + j) % n_tp, ssem, rsem)

    def source(k):
        return (my_chip + chips - turn(k)) % chips

    def give_back(chip, core):
        return remote(
            prod.at[chip, core],
            out.at[my_chip, my_core],
            r_send.at[chip * CORES + core],
            r_recv.at[sp],
            (chip * CORES + core, tp),
        )

    tile = min(hidden, 256)
    wide = min(cols, 256)

    @pl.loop(0, chips + 4)
    def _(i):
        @pl.when(i < chips)
        def _():
            chip = source(i)
            for core in range(CORES):
                remote(
                    send.at[chip, core],
                    rows.at[chip, tp, core],
                    d_send.at[0],
                    d_recv.at[chip * CORES + core],
                    (sp, tp),
                ).wait_recv()
            for copy in spread(rows, chip, f_send, f_recv):
                copy.start()

        @pl.when((i >= 1) & (i < chips + 1))
        def _():
            pass_on(rows, source(i - 1), f_send, f_recv)

        @pl.when(i == 2)
        def _():
            for copy in loads:
                copy.wait()

        @pl.when((i >= 2) & (i < chips + 2))
        def _():
            chip = source(i - 2)
            complete(rows, chip, f_send, f_recv)

            @pl.loop(0, hidden // tile)
            def _(n):
                at = pl.ds(pl.multiple_of(n * tile, tile), tile)
                gate = jnp.zeros((flat, tile), jnp.float32)
                up = jnp.zeros((flat, tile), jnp.float32)
                for t in range(n_tp):
                    block = rows[chip, t].reshape(flat, cols)
                    deep = pl.ds(t * cols, cols)
                    gate += jnp.dot(block, w_gate[deep, at], preferred_element_type=jnp.float32)
                    up += jnp.dot(block, w_up[deep, at], preferred_element_type=jnp.float32)
                value = (jax.nn.silu(gate) * up).astype(jnp.bfloat16)
                act[chip, tp, :, :, at] = value.reshape(CORES, cap, tile)

            for copy in spread(act, chip, a_send, a_recv):
                copy.start()

        @pl.when((i >= 3) & (i < chips + 3))
        def _():
            pass_on(act, source(i - 3), a_send, a_recv)

        @pl.when(i >= 4)
        def _():
            chip = source(i - 4)
            complete(act, chip, a_send, a_recv)

            @pl.loop(0, cols // wide)
            def _(n):
                at = pl.ds(pl.multiple_of(n * wide, wide), wide)
                total = jnp.zeros((flat, wide), jnp.float32)
                for t in range(n_tp):
                    block = act[chip, t].reshape(flat, hidden)
                    total += jnp.dot(
                        block, w_down[pl.ds(t * hidden, hidden), at], preferred_element_type=jnp.float32
                    )
                prod[chip, :, :, at] = total.astype(jnp.bfloat16).reshape(CORES, cap, wide)

            @pl.when(i == 4)
            def _():
                pltpu.make_async_copy(
                    prod.at[my_chip, my_core], out.at[my_chip, my_core], r_recv.at[sp]
                ).start()
                give_back(my_chip, 1 - my_core).start()

            @pl.when(i > 4)
            def _():
                for core in range(CORES):
                    give_back(chip, core).start()

    dispatch(my_chip, 1 - my_core).wait_send()
    give_back(my_chip, 1 - my_core).wait_send()

    @pl.loop(1, chips)
    def _(k):
        chip = (my_chip + turn(k)) % chips
        for core in range(CORES):
            dispatch(chip, core).wait_send()
            give_back(chip, core).wait_send()

    @pl.loop(0, chips)
    def _(chip):
        for buf, ssem, rsem in ((rows, f_send, f_recv), (act, a_send, a_recv)):
            for copy in spread(buf, chip, ssem, rsem):
                copy.wait_send()
            if relay:
                for copy in relays(buf, chip, ssem, rsem):
                    copy.wait_send()
        for core in range(CORES):
            remote(
                prod.at[chip, core],
                out.at[chip, core],
                r_send.at[0],
                r_recv.at[chip * CORES + core],
                (sp, tp),
            ).wait_recv()


VMEM_LIMIT = 60 * 1024 * 1024


def project(pooled, residual, gain, weight):
    n_tp = lax.axis_size("tp")
    length, cols = residual.shape
    dma = pltpu.SemaphoreType.DMA
    vmem = pl.BlockSpec(memory_space=pltpu.VMEM)
    return pl.pallas_call(
        functools.partial(project_kernel, n_tp),
        out_shape=[jax.ShapeDtypeStruct((length, cols), jnp.bfloat16)] * 2,
        in_specs=[vmem, vmem, vmem, pl.BlockSpec(memory_space=pl.ANY)],
        out_specs=[vmem, vmem],
        scratch_shapes=[
            pltpu.VMEM((n_tp, *pooled.shape), jnp.bfloat16),
            pltpu.VMEM(weight.shape, jnp.bfloat16),
            pltpu.VMEM((8, length), jnp.float32),
            pltpu.VMEM((n_tp, 8, length), jnp.float32),
            dma,
            dma((n_tp,)),
            dma((n_tp,)),
            dma((n_tp,)),
            dma((n_tp,)),
        ],
        compiler_params=pltpu.CompilerParams(
            collective_id=0, has_side_effects=True, vmem_limit_bytes=VMEM_LIMIT
        ),
    )(pooled, residual, gain, weight)


def run_experts(send, w_gate, w_up, w_down):
    n_sp, n_tp = lax.axis_size("sp"), lax.axis_size("tp")
    chips, _, cap, cols = send.shape
    hidden = w_gate.shape[1]
    dma = pltpu.SemaphoreType.DMA
    vmem = pl.BlockSpec(memory_space=pltpu.VMEM)
    hbm = pl.BlockSpec(memory_space=pl.ANY)
    return pl.pallas_call(
        functools.partial(experts_kernel, n_sp, n_tp),
        out_shape=jax.ShapeDtypeStruct(send.shape, jnp.bfloat16),
        in_specs=[vmem, hbm, hbm, hbm],
        out_specs=vmem,
        scratch_shapes=[
            pltpu.VMEM((chips, n_tp, CORES, cap, cols), jnp.bfloat16),
            pltpu.VMEM((chips, n_tp, CORES, cap, hidden), jnp.bfloat16),
            pltpu.VMEM(send.shape, jnp.bfloat16),
            pltpu.VMEM(w_gate.shape, jnp.bfloat16),
            pltpu.VMEM(w_up.shape, jnp.bfloat16),
            pltpu.VMEM(w_down.shape, jnp.bfloat16),
            dma((3,)),
            dma((n_sp,)),
            dma((n_sp,)),
            dma((chips, n_tp)),
            dma((chips, n_tp + 2)),
            dma((chips, n_tp)),
            dma((chips, n_tp + 2)),
            dma((n_sp,)),
            dma((n_sp,)),
        ],
        compiler_params=pltpu.CompilerParams(
            collective_id=1, has_side_effects=True, vmem_limit_bytes=VMEM_LIMIT
        ),
    )(send, w_gate, w_up, w_down)


def shards(
    residual,
    pool_in,
    docs,
    pool_weight,
    pool_gain,
    out_weight,
    norm_gain,
    routes,
    route_weights,
    w_gate,
    w_up,
    w_down,
):
    length = pool_in.shape[0]
    width_loc = pool_in.shape[1]
    sp_index = lax.axis_index("sp")
    tp_index = lax.axis_index("tp")
    n_sp = lax.axis_size("sp")
    n_tp = lax.axis_size("tp")
    reach = 15
    prev_rows, prev_docs = shifted_2(
        (pool_in[length - reach :], docs[length - reach :].astype(jnp.bfloat16)), "sp", 1
    )
    extended = jnp.concatenate([prev_rows, pool_in], axis=0).astype(jnp.float32)
    ext_docs = jnp.concatenate([prev_docs.astype(jnp.float32), docs.astype(jnp.float32)])
    own_docs = docs.astype(jnp.float32)
    places = sp_index * length + jnp.arange(length)
    groups_loc = width_loc // GD
    group_of = tp_index * groups_loc + jnp.arange(width_loc) // GD
    span = 2 ** (1 + group_of % 4)
    totals = jnp.zeros((length, width_loc), jnp.float32)
    counts = jnp.zeros((length, width_loc), jnp.float32)
    for offset in range(16):
        shifted = extended[reach - offset : reach - offset + length]
        prior = ext_docs[reach - offset : reach - offset + length]
        same = ((places >= offset) & (prior == own_docs)).astype(jnp.float32)[:, None]
        weight = same * (offset < span).astype(jnp.float32)[None, :]
        totals = totals + weight * shifted
        counts = counts + weight
    diff = (totals / counts - extended[reach:]).astype(jnp.bfloat16)
    mixed = jnp.einsum(
        "tgc,gcd->tgd",
        diff.reshape(length, groups_loc, GD),
        pool_weight,
        preferred_element_type=jnp.float32,
    )
    pooled = (mixed.reshape(length, width_loc) * pool_gain).astype(jnp.bfloat16)
    cols = residual.shape[1]
    experts = n_sp * EXP_DEV
    slots_cap = length * TOPK * 3 // (2 * experts)
    ids = routes.reshape(-1)
    onehot = (ids[:, None] == jnp.arange(experts)[None, :]).astype(jnp.int32)
    rank = jnp.sum(onehot * (jnp.cumsum(onehot, axis=0) - 1), axis=1)
    slot = (ids * slots_cap + rank).reshape(length, TOPK)
    gain_cols = lax.dynamic_slice_in_dim(norm_gain, tp_index * cols, cols, 0)
    updated, normed = project(pooled, residual, gain_cols[None, :], out_weight)
    places_all = jnp.arange(experts * slots_cap)
    picks = [(slot[:, k : k + 1] == places_all[None, :]).astype(jnp.bfloat16) for k in range(TOPK)]
    send = lax.dot_general(
        sum(picks), normed, (((0,), (0,)), ((), ())), preferred_element_type=jnp.float32
    ).astype(jnp.bfloat16)
    returned = run_experts(
        send.reshape(n_sp // CORES, CORES, slots_cap, cols), w_gate[0], w_up[0], w_down[0]
    ).reshape(-1, cols)
    total = jnp.zeros((length, cols), jnp.float32)
    for k in range(TOPK):
        row = jnp.dot(picks[k], returned, preferred_element_type=jnp.float32)
        total = total + route_weights[:, k : k + 1] * row
    combined = updated.astype(jnp.float32) + total
    return combined.astype(jnp.bfloat16)


def solution(mesh):
    placed = (
        P("sp", "tp"),
        P("sp", "tp"),
        P("sp"),
        P("tp", None, None),
        P("tp"),
        P(None, "tp"),
        P(),
        P("sp", None),
        P("sp", None),
        P("sp", None, "tp"),
        P("sp", None, "tp"),
        P("sp", None, "tp"),
    )
    return jax.shard_map(
        shards, mesh=mesh, in_specs=placed, out_specs=P("sp", "tp"), check_vma=False
    )
```
